32 devices in a mesh: rep: 4 (over z), fs: 4 (over y, x), tp: 2 (over core).
Axes of the slice: x: 2, y: 2, z: 4, core: 2. Of those that a mesh axis runs over, the one named last changes fastest.
Arguments:
- tokens_in: bfloat16 [3072, 1024], P(('rep', 'fs', 'tp')), may hold values from -6 to 6
- out_grad: bfloat16 [3072, 1024], P(('rep', 'fs', 'tp')), may hold values from -6 to 6
- gate_weight: bfloat16 [1024, 2816], P('fs', 'tp'), may hold values from -0.1875 to 0.1875
- up_weight: bfloat16 [1024, 2816], P('fs', 'tp'), may hold values from -0.1875 to 0.1875
- down_weight: bfloat16 [2816, 1024], P('tp', 'fs'), may hold values from -0.109375 to 0.109375
Outputs:
- grad_in: bfloat16 [3072, 1024], P(('rep', 'fs', 'tp'))
- grad_gate_w: float32 [1024, 2816], P('fs', 'tp')
- grad_up_w: float32 [1024, 2816], P('fs', 'tp')
- grad_down_w: float32 [2816, 1024], P('tp', 'fs')
The draws below stay inside these ranges and needn't reach their ends.
All inputs are finite; a program needn't handle non-finite values.
Results may differ from the reference program's by a relative error of at most 0.02.
Values may be sent and summed in bfloat16 or wider, within the bound.
A program may use at most 64 MiB of HBM per device.

```python
import jax
import jax.numpy as jnp

D = 1024
FF = 2816
TOKENS = 3072


def raised(result, rng, source, target, shards_of, factor):
    def block_of(dim):
        return (jnp.arange(result.shape[dim]) // (result.shape[dim] // shards_of)).reshape((-1,) + (1,) * (result.ndim - 1 - dim))

    first = jax.random.permutation(rng, shards_of)[block_of(target)]
    other_side = (block_of(target) + shards_of // 2) % shards_of
    return jnp.where((block_of(source) == first) | (block_of(source) == other_side), factor * result, result)


def steps_of(stream_key, shape, cuts, least, largest):
    factor_of = 1.0
    for axis_at, parts in cuts:
        heights = jax.random.uniform(jax.random.fold_in(jax.random.fold_in(stream_key, 6), axis_at), (parts,), jnp.float32, least / len(cuts), largest / len(cuts))
        factor_of = factor_of * jnp.repeat(jnp.exp(heights), shape[axis_at] // parts).reshape((-1,) + (1,) * (len(shape) - 1 - axis_at))
    return factor_of


def bell_draw(stream_key, dims, scale, limit, pieces=(), dtype=jnp.bfloat16):
    entries = scale * jax.random.normal(stream_key, dims, jnp.float32)
    if pieces:
        entries = entries * steps_of(stream_key, dims, pieces, -0.22, 0.18)
    return jnp.clip(entries, -limit, limit).astype(dtype)


def noise_with(stream_key, extent, deviation, limit, split, heavy, dtype=jnp.bfloat16):
    values = deviation * jax.random.normal(stream_key, extent, jnp.float32)
    if split:
        values = values * steps_of(stream_key, extent, split, -0.22, 0.18)
    return jnp.clip(raised(values, jax.random.fold_in(stream_key, 3), *heavy), -limit, limit).astype(dtype)


def setup_inputs(seed: int = 0) -> dict:
    arg_keys = jax.random.split(jax.random.key(seed), 6)
    tokens_in = bell_draw(arg_keys[0], (TOKENS, D), 1.0, 6.0, ((0, 32),))
    out_grad = noise_with(arg_keys[1], (TOKENS, D), 1.0, 6.0, ((0, 32),), (0, 1, 32, 2.75))
    gate_weight = bell_draw(arg_keys[2], (D, FF), D ** -0.5, 0.1875, ((0, 4), (1, 2)))
    up_weight = bell_draw(arg_keys[3], (D, FF), D ** -0.5, 0.1875, ((0, 4), (1, 2)))
    down_weight = bell_draw(arg_keys[4], (FF, D), FF ** -0.5, 0.109375, ((0, 2), (1, 4)))
    return dict(tokens_in=tokens_in, out_grad=out_grad, gate_weight=gate_weight, up_weight=up_weight, down_weight=down_weight)


def reference(tokens_in, out_grad, gate_weight, up_weight, down_weight):
    gate = jnp.dot(tokens_in, gate_weight, preferred_element_type=jnp.float32).astype(jnp.bfloat16)
    up_proj = jnp.dot(tokens_in, up_weight, preferred_element_type=jnp.float32).astype(jnp.bfloat16)
    gate_wide = gate.astype(jnp.float32)
    up_wide = up_proj.astype(jnp.float32)
    sigmoid = jax.nn.sigmoid(gate_wide)
    activated = gate_wide * sigmoid
    hidden = (activated * up_wide).astype(jnp.bfloat16)
    grad_hidden = jnp.dot(out_grad, down_weight.T, preferred_element_type=jnp.float32).astype(jnp.bfloat16)
    grad_wide = grad_hidden.astype(jnp.float32)
    grad_gate = (grad_wide * up_wide * sigmoid * (1.0 + gate_wide * (1.0 - sigmoid))).astype(jnp.bfloat16)
    grad_up = (grad_wide * activated).astype(jnp.bfloat16)
    grad_in = (jnp.dot(grad_gate, gate_weight.T, preferred_element_type=jnp.float32)
               + jnp.dot(grad_up, up_weight.T, preferred_element_type=jnp.float32)).astype(jnp.bfloat16)
    factor = TOKENS ** -0.5
    grad_gate_w = jnp.dot(tokens_in.T, grad_gate, preferred_element_type=jnp.float32) * factor
    grad_up_w = jnp.dot(tokens_in.T, grad_up, preferred_element_type=jnp.float32) * factor
    grad_down_w = jnp.dot(hidden.T, out_grad, preferred_element_type=jnp.float32) * factor
    return grad_in, grad_gate_w, grad_up_w, grad_down_w
```

```python
import jax
import jax.numpy as jnp
from jax import lax
from jax.sharding import PartitionSpec as P


def contract_last(left, right):
    return lax.dot_general(
        left, right, (((1,), (1,)), ((), ())), preferred_element_type=jnp.float32
    )


def contract_first(left, right):
    return lax.dot_general(
        left, right, (((0,), (0,)), ((), ())), preferred_element_type=jnp.float32
    )


def body(tokens_in, out_grad, gate_weight, up_weight, down_weight):
    replicas = lax.axis_size("rep")
    shards = lax.axis_size("fs")
    columns = lax.axis_size("tp")
    local_rows = tokens_in.shape[0]
    hidden_cols = gate_weight.shape[1]
    factor = (local_rows * replicas * shards * columns) ** (-0.5)
    part = hidden_cols // replicas
    offset = lax.axis_index("rep") * part
    pieces = jnp.stack(
        [
            lax.dynamic_slice_in_dim(gate_weight, offset, part, 1).T,
            lax.dynamic_slice_in_dim(up_weight, offset, part, 1).T,
            lax.dynamic_slice_in_dim(down_weight, offset, part, 0),
        ]
    )
    full = lax.all_gather(pieces, "fs", axis=2, tiled=True)
    gate_full, up_full, down_full = full[0], full[1], full[2]
    both = lax.all_gather(jnp.stack([tokens_in, out_grad]), ("rep", "tp"), axis=1, tiled=True)
    tokens_all, grads_all = both[0], both[1]
    gate = contract_last(tokens_all, gate_full).astype(jnp.bfloat16)
    up_proj = contract_last(tokens_all, up_full).astype(jnp.bfloat16)
    gate_wide = gate.astype(jnp.float32)
    up_wide = up_proj.astype(jnp.float32)
    sigmoid = jax.nn.sigmoid(gate_wide)
    activated = gate_wide * sigmoid
    hidden = (activated * up_wide).astype(jnp.bfloat16)
    grad_hidden = contract_last(grads_all, down_full).astype(jnp.bfloat16)
    grad_wide = grad_hidden.astype(jnp.float32)
    grad_gate = (grad_wide * up_wide * sigmoid * (1.0 + gate_wide * (1.0 - sigmoid))).astype(
        jnp.bfloat16
    )
    grad_up = (grad_wide * activated).astype(jnp.bfloat16)
    weights = factor * jnp.stack(
        [
            contract_first(grad_gate, tokens_all),
            contract_first(grad_up, tokens_all),
            contract_first(hidden, grads_all),
        ]
    )
    owned = lax.psum_scatter(
        weights.astype(jnp.bfloat16), "fs", scatter_dimension=2, tiled=True
    )
    summed = lax.all_gather(owned, "rep", axis=1, tiled=True).astype(jnp.float32)
    partial = jnp.dot(grad_gate, gate_full, preferred_element_type=jnp.float32) + jnp.dot(
        grad_up, up_full, preferred_element_type=jnp.float32
    )
    grad_in = lax.psum_scatter(
        partial.astype(jnp.bfloat16), ("rep", "tp"), scatter_dimension=0, tiled=True
    )
    return (grad_in, summed[0].T, summed[1].T, summed[2])


def solution(mesh):
    placed = (
        P(("rep", "fs", "tp"), None),
        P(("rep", "fs", "tp"), None),
        P("fs", "tp"),
        P("fs", "tp"),
        P("tp", "fs"),
    )
    return jax.shard_map(
        body,
        mesh=mesh,
        in_specs=placed,
        out_specs=(P(("rep", "fs", "tp"), None), P("fs", "tp"), P("fs", "tp"), P("tp", "fs")),
        check_vma=False,
    )
```

```python
import functools

import jax
import jax.numpy as jnp
from jax import lax
from jax.experimental import pallas as pl
from jax.experimental.pallas import tpu as pltpu
from jax.sharding import PartitionSpec as P

BF = jnp.bfloat16
F32 = jnp.float32
MESH = pl.DeviceIdType.MESH


def ring_order(index):
    return index + (index // 2) * (5 - 2 * index)


def kernel(
    columns,
    factor,
    tokens_ref,
    grads_ref,
    w_ref,
    gin_ref,
    gw_ref,
    T,
    W,
    H,
    S,
    O,
    RD,
    RR,
    G,
    PS,
    PR,
    Q,
    QR,
    w_send,
    w_recv,
    t_send,
    t_recv,
    c_send,
    c_recv,
    d_send,
    d_recv,
    s_send,
    s_recv,
    g_send,
    g_recv,
    p_send,
    p_recv,
    q_send,
    q_recv,
):
    rep = lax.axis_index("rep")
    fs = lax.axis_index("fs")
    tp = lax.axis_index("tp")
    rows = tokens_ref.shape[0]
    width = w_ref.shape[2]
    half = width // 2
    tile = 4 * rows
    spot = ring_order(fs)
    near = [ring_order(lax.rem(spot + k, 4)) for k in range(4)]
    level = [lax.rem(rep + k, 4) for k in range(4)]
    core = [lax.rem(tp + k, columns) for k in range(columns)]

    def to_fs(k):
        return (rep, near[k], tp)

    def to_rep(k):
        return (level[k], fs, tp)

    def to_tp(k):
        return (rep, fs, core[k])

    peers = [to_fs(k) for k in (1, 2, 3)] + [to_rep(k) for k in (1, 2, 3)]
    peers += [to_tp(k) for k in range(1, columns)]
    barrier = pltpu.get_barrier_semaphore()
    for peer in peers:
        pl.semaphore_signal(barrier, inc=1, device_id=peer, device_id_type=MESH)
    pl.semaphore_wait(barrier, len(peers))

    pending = []

    def send(src, dst, send_sem, recv_sem, device):
        copy = pltpu.make_async_remote_copy(
            src_ref=src, dst_ref=dst, send_sem=send_sem, recv_sem=recv_sem,
            device_id=device, device_id_type=MESH,
        )
        copy.start()
        pending.append(copy)

    def arrive(dst, send_sem, recv_sem, device):
        pltpu.make_async_remote_copy(
            src_ref=dst, dst_ref=dst, send_sem=send_sem, recv_sem=recv_sem,
            device_id=device, device_id_type=MESH,
        ).wait_recv()

    sides = (1, 3)

    def lanes(side):
        return pl.ds(side * half, half)

    def block(kind, column, row):
        start = pl.multiple_of((column * 4 + row) * rows, rows)
        return T.at[kind, pl.ds(start, rows), :]

    mine = (tokens_ref, grads_ref)
    for kind in range(2):
        for side in range(2):
            send(mine[kind], block(kind, tp, rep), t_send.at[0, kind, side],
                 t_recv.at[0, kind, side], to_rep(sides[side]))
    for w in range(3):
        for side in range(2):
            send(w_ref.at[w], W.at[fs, w], w_send.at[0, w, side], w_recv.at[0, w, side],
                 to_fs(sides[side]))

    def share(kind, k):
        for j in range(1, columns):
            if k == 0:
                src = mine[kind]
            else:
                src = block(kind, tp, level[k])
            send(src, block(kind, tp, level[k]), c_send.at[j, kind, k], c_recv.at[j, kind, k],
                 to_tp(j))

    for kind in range(2):
        share(kind, 0)
        T[kind, pl.ds(pl.multiple_of((tp * 4 + rep) * rows, rows), rows), :] = mine[kind][...]
    W[fs] = w_ref[...]

    for kind in range(2):
        for side in range(2):
            k = 4 - sides[side]
            arrive(block(kind, tp, level[k]), t_send.at[0, kind, side],
                   t_recv.at[0, kind, side], to_rep(sides[side]))
            if kind == side:
                send(block(kind, tp, level[k]), block(kind, tp, level[k]),
                     t_send.at[1, kind, side], t_recv.at[1, kind, side], to_rep(sides[side]))
            share(kind, k)
    for w in range(3):
        for side in range(2):
            f = near[4 - sides[side]]
            arrive(W.at[f, w], w_send.at[0, w, side], w_recv.at[0, w, side], to_fs(sides[side]))
            send(W.at[f, w, :, lanes(side)], W.at[f, w, :, lanes(side)],
                 w_send.at[1, w, side], w_recv.at[1, w, side], to_fs(sides[side]))
    for kind in range(2):
        arrive(block(kind, tp, level[2]), t_send.at[1, kind, kind], t_recv.at[1, kind, kind],
               to_rep(sides[kind]))
        share(kind, 2)
    for kind in range(2):
        for k in range(4):
            for j in range(1, columns):
                arrive(block(kind, core[columns - j], level[k]), c_send.at[j, kind, k],
                       c_recv.at[j, kind, k], to_tp(j))
    for w in range(3):
        for side in range(2):
            arrive(W.at[near[2], w, :, lanes(side)], w_send.at[1, w, side],
                   w_recv.at[1, w, side], to_fs(sides[side]))

    def product(kind, w, at):
        total = None
        for f in range(4):
            piece = lax.dot_general(
                T[kind, at, f * width : (f + 1) * width], W[f, w],
                (((1,), (1,)), ((), ())), preferred_element_type=F32,
            )
            total = piece if total is None else total + piece
        return total.astype(BF).astype(F32)

    def activations(i, carry):
        at = pl.ds(pl.multiple_of(i * tile, tile), tile)
        gate = product(0, 0, at)
        up = product(0, 1, at)
        sigmoid = jax.nn.sigmoid(gate)
        activated = gate * sigmoid
        H[2, at, :] = (activated * up).astype(BF)
        grad = product(1, 2, at)
        H[0, at, :] = (grad * up * sigmoid * (1.0 + gate * (1.0 - sigmoid))).astype(BF)
        H[1, at, :] = (grad * activated).astype(BF)
        return carry

    lax.fori_loop(0, columns, activations, 0)

    def weight_part(w, k):
        at = pl.ds(pl.multiple_of(near[k] * width, width), width)
        return factor * lax.dot_general(
            H[w], T[1 if w == 2 else 0, :, at], (((0,), (0,)), ((), ())),
            preferred_element_type=F32,
        )

    for w in range(3):
        far = weight_part(w, 2).astype(BF)
        for side in range(2):
            S[w, 0, side] = far[:, side * half : (side + 1) * half]
            send(S.at[w, 0, side], RD.at[w, side], d_send.at[w, side], d_recv.at[w, side],
                 to_fs(sides[side]))
        for side in range(2):
            part = weight_part(w, sides[side]).astype(BF)
            for h in range(2):
                S[w, 1 + side, h] = part[:, h * half : (h + 1) * half]
            h = 1 - side
            send(S.at[w, 1 + side, h], RR.at[w, side, h], s_send.at[w, side, h],
                 s_recv.at[w, side, h], to_fs(sides[side]))
        O[w] = weight_part(w, 0)

    def input_part(i, f):
        at = pl.ds(pl.multiple_of(i * tile, tile), tile)
        return jnp.dot(H[0, at, :], W[f, 0], preferred_element_type=F32) + jnp.dot(
            H[1, at, :], W[f, 1], preferred_element_type=F32
        )

    for j in range(1, columns):
        for f in range(4):
            PS[j, :, f * width : (f + 1) * width] = input_part(core[j], f).astype(BF)
        send(PS.at[j], PR.at[j], p_send.at[j], p_recv.at[j], to_tp(j))

    for w in range(3):
        for side in range(2):
            arrive(RD.at[w, side], d_send.at[w, side], d_recv.at[w, side], to_fs(sides[side]))
            S[w, 3 + side, side] = (
                S[w, 1 + side, side].astype(F32) + RD[w, side].astype(F32)
            ).astype(BF)
            send(S.at[w, 3 + side, side], RR.at[w, side, side], s_send.at[w, side, side],
                 s_recv.at[w, side, side], to_fs(sides[side]))

    for j in range(1, columns):
        arrive(PR.at[j], p_send.at[j], p_recv.at[j], to_tp(j))
    for f in range(4):
        at = slice(f * width, (f + 1) * width)
        total = input_part(tp, f)
        for j in range(1, columns):
            total += PR[j, :, at].astype(F32)
        for r in range(4):
            Q[r, :, at] = total[r * rows : (r + 1) * rows].astype(BF)
    for k in (2, 1, 3):
        send(Q.at[level[k]], QR.at[k], q_send.at[k], q_recv.at[k], to_rep(k))

    for w in range(3):
        for side in range(2):
            for h in range(2):
                arrive(RR.at[w, side, h], s_send.at[w, side, h], s_recv.at[w, side, h],
                       to_fs(sides[side]))
        for h in range(2):
            at = slice(h * half, (h + 1) * half)
            G[rep, w, :, at] = (
                O[w, :, at] + RR[w, 0, h].astype(F32) + RR[w, 1, h].astype(F32)
            ).astype(BF)
        for side in range(2):
            send(G.at[rep, w], G.at[rep, w], g_send.at[0, w, side], g_recv.at[0, w, side],
                 to_rep(sides[side]))

    for k in (1, 2, 3):
        arrive(QR.at[k], q_send.at[k], q_recv.at[k], to_rep(k))
    total = Q[rep].astype(F32)
    for k in (1, 2, 3):
        total += QR[k].astype(F32)
    gin_ref[...] = total.astype(BF)

    for w in range(3):
        for side in range(2):
            r = level[4 - sides[side]]
            arrive(G.at[r, w], g_send.at[0, w, side], g_recv.at[0, w, side], to_rep(sides[side]))
            send(G.at[r, w, :, lanes(side)], G.at[r, w, :, lanes(side)],
                 g_send.at[1, w, side], g_recv.at[1, w, side], to_rep(sides[side]))
    for w in range(3):
        for side in range(2):
            arrive(G.at[level[2], w, :, lanes(side)], g_send.at[1, w, side],
                   g_recv.at[1, w, side], to_rep(sides[side]))
        for r in range(4):
            gw_ref[w, r] = G[r, w]
    for copy in pending:
        copy.wait_send()


def body(tokens_in, out_grad, gate_weight, up_weight, down_weight):
    replicas = lax.axis_size("rep")
    shards = lax.axis_size("fs")
    columns = lax.axis_size("tp")
    rows, model = tokens_in.shape
    width, hidden_cols = gate_weight.shape
    everyone = rows * replicas * columns
    factor = (everyone * shards) ** (-0.5)
    part = hidden_cols // replicas
    half = width // 2
    offset = lax.axis_index("rep") * part
    pieces = jnp.stack(
        [
            lax.dynamic_slice_in_dim(gate_weight, offset, part, 1).T,
            lax.dynamic_slice_in_dim(up_weight, offset, part, 1).T,
            lax.dynamic_slice_in_dim(down_weight, offset, part, 0),
        ]
    )
    sems = pltpu.SemaphoreType.DMA
    shapes = []
    for dims in ((2, 3, 2), (2, 2, 2), (columns, 2, 4), (3, 2), (3, 2, 2), (2, 3, 2), (columns,), (4,)):
        shapes += [sems(dims), sems(dims)]
    vmem = pl.BlockSpec(memory_space=pltpu.VMEM)
    grad_in, summed = pl.pallas_call(
        functools.partial(kernel, columns, factor),
        out_shape=(
            jax.ShapeDtypeStruct((rows, model), BF),
            jax.ShapeDtypeStruct((3, 4, part, width), BF),
        ),
        in_specs=[vmem] * 3,
        out_specs=(vmem, vmem),
        scratch_shapes=[
            pltpu.VMEM((2, everyone, model), BF),
            pltpu.VMEM((4, 3, part, width), BF),
            pltpu.VMEM((3, everyone, part), BF),
            pltpu.VMEM((3, 5, 2, part, half), BF),
            pltpu.VMEM((3, part, width), F32),
            pltpu.VMEM((3, 2, part, half), BF),
            pltpu.VMEM((3, 2, 2, part, half), BF),
            pltpu.VMEM((4, 3, part, width), BF),
            pltpu.VMEM((columns, 4 * rows, model), BF),
            pltpu.VMEM((columns, 4 * rows, model), BF),
            pltpu.VMEM((4, rows, model), BF),
            pltpu.VMEM((4, rows, model), BF),
        ]
        + shapes,
        compiler_params=pltpu.CompilerParams(
            collective_id=0, has_side_effects=True, vmem_limit_bytes=60 * 1024 * 1024
        ),
    )(tokens_in, out_grad, pieces)
    wide = summed.reshape(3, hidden_cols, width).astype(F32)
    return (grad_in, wide[0].T, wide[1].T, wide[2])


def contract_last(left, right):
    return lax.dot_general(
        left, right, (((1,), (1,)), ((), ())), preferred_element_type=jnp.float32
    )


def contract_first(left, right):
    return lax.dot_general(
        left, right, (((0,), (0,)), ((), ())), preferred_element_type=jnp.float32
    )


def plain_body(tokens_in, out_grad, gate_weight, up_weight, down_weight):
    replicas = lax.axis_size("rep")
    shards = lax.axis_size("fs")
    columns = lax.axis_size("tp")
    local_rows = tokens_in.shape[0]
    hidden_cols = gate_weight.shape[1]
    factor = (local_rows * replicas * shards * columns) ** (-0.5)
    part = hidden_cols // replicas
    offset = lax.axis_index("rep") * part
    pieces = jnp.stack(
        [
            lax.dynamic_slice_in_dim(gate_weight, offset, part, 1).T,
            lax.dynamic_slice_in_dim(up_weight, offset, part, 1).T,
            lax.dynamic_slice_in_dim(down_weight, offset, part, 0),
        ]
    )
    full = lax.all_gather(pieces, "fs", axis=2, tiled=True)
    gate_full, up_full, down_full = full[0], full[1], full[2]
    both = lax.all_gather(jnp.stack([tokens_in, out_grad]), ("rep", "tp"), axis=1, tiled=True)
    tokens_all, grads_all = both[0], both[1]
    gate = contract_last(tokens_all, gate_full).astype(jnp.bfloat16)
    up_proj = contract_last(tokens_all, up_full).astype(jnp.bfloat16)
    gate_wide = gate.astype(jnp.float32)
    up_wide = up_proj.astype(jnp.float32)
    sigmoid = jax.nn.sigmoid(gate_wide)
    activated = gate_wide * sigmoid
    hidden = (activated * up_wide).astype(jnp.bfloat16)
    grad_hidden = contract_last(grads_all, down_full).astype(jnp.bfloat16)
    grad_wide = grad_hidden.astype(jnp.float32)
    grad_gate = (grad_wide * up_wide * sigmoid * (1.0 + gate_wide * (1.0 - sigmoid))).astype(
        jnp.bfloat16
    )
    grad_up = (grad_wide * activated).astype(jnp.bfloat16)
    weights = factor * jnp.stack(
        [
            contract_first(grad_gate, tokens_all),
            contract_first(grad_up, tokens_all),
            contract_first(hidden, grads_all),
        ]
    )
    owned = lax.psum_scatter(
        weights.astype(jnp.bfloat16), "fs", scatter_dimension=2, tiled=True
    )
    summed = lax.all_gather(owned, "rep", axis=1, tiled=True).astype(jnp.float32)
    partial = jnp.dot(grad_gate, gate_full, preferred_element_type=jnp.float32) + jnp.dot(
        grad_up, up_full, preferred_element_type=jnp.float32
    )
    grad_in = lax.psum_scatter(
        partial.astype(jnp.bfloat16), ("rep", "tp"), scatter_dimension=0, tiled=True
    )
    return (grad_in, summed[0].T, summed[1].T, summed[2])


def solution(mesh):
    placed = (
        P(("rep", "fs", "tp"), None),
        P(("rep", "fs", "tp"), None),
        P("fs", "tp"),
        P("fs", "tp"),
        P("tp", "fs"),
    )
    fits = mesh.shape["rep"] == 4 and mesh.shape["fs"] == 4
    return jax.shard_map(
        body if fits else plain_body,
        mesh=mesh,
        in_specs=placed,
        out_specs=(P(("rep", "fs", "tp"), None), P("fs", "tp"), P("fs", "tp"), P("tp", "fs")),
        check_vma=False,
    )
```

```python
import functools

import jax
import jax.numpy as jnp
from jax import lax
from jax.experimental import pallas as pl
from jax.experimental.pallas import tpu as pltpu
from jax.sharding import PartitionSpec as P

BF = jnp.bfloat16
F32 = jnp.float32
MESH = pl.DeviceIdType.MESH


def ring_order(index):
    return index + (index // 2) * (5 - 2 * index)


def kernel(
    columns,
    factor,
    tokens_ref,
    grads_ref,
    w_ref,
    gin_ref,
    gu_ref,
    gd_ref,
    T,
    W,
    H,
    S,
    O,
    RD,
    RR,
    G,
    PS,
    PR,
    Q,
    QR,
    w_send,
    w_recv,
    t_send,
    t_recv,
    c_send,
    c_recv,
    d_send,
    d_recv,
    s_send,
    s_recv,
    g_send,
    g_recv,
    p_send,
    p_recv,
    q_send,
    q_recv,
):
    rep = lax.axis_index("rep")
    fs = lax.axis_index("fs")
    tp = lax.axis_index("tp")
    rows = tokens_ref.shape[0]
    width = w_ref.shape[2]
    part = w_ref.shape[1]
    half = width // 2
    tile = 4 * rows
    spot = ring_order(fs)
    near = [ring_order(lax.rem(spot + k, 4)) for k in range(4)]
    level = [lax.rem(rep + k, 4) for k in range(4)]
    core = [lax.rem(tp + k, columns) for k in range(columns)]

    def to_fs(k):
        return (rep, near[k], tp)

    def to_rep(k):
        return (level[k], fs, tp)

    def to_tp(k):
        return (rep, fs, core[k])

    peers = [to_fs(k) for k in (1, 2, 3)] + [to_rep(k) for k in (1, 2, 3)]
    peers += [to_tp(k) for k in range(1, columns)]
    barrier = pltpu.get_barrier_semaphore()
    for peer in peers:
        pl.semaphore_signal(barrier, inc=1, device_id=peer, device_id_type=MESH)
    pl.semaphore_wait(barrier, len(peers))

    pending = []

    def send(src, dst, send_sem, recv_sem, device):
        copy = pltpu.make_async_remote_copy(
            src_ref=src, dst_ref=dst, send_sem=send_sem, recv_sem=recv_sem,
            device_id=device, device_id_type=MESH,
        )
        copy.start()
        pending.append(copy)

    def arrive(dst, send_sem, recv_sem, device):
        pltpu.make_async_remote_copy(
            src_ref=dst, dst_ref=dst, send_sem=send_sem, recv_sem=recv_sem,
            device_id=device, device_id_type=MESH,
        ).wait_recv()

    sides = (1, 3)

    def lanes(side):
        return pl.ds(side * half, half)

    def block(kind, column, row):
        start = pl.multiple_of((column * 4 + row) * rows, rows)
        return T.at[kind, pl.ds(start, rows), :]

    mine = (tokens_ref, grads_ref)
    for kind in range(2):
        for side in range(2):
            send(mine[kind], block(kind, tp, rep), t_send.at[0, kind, side],
                 t_recv.at[0, kind, side], to_rep(sides[side]))
    for w in range(3):
        for side in range(2):
            send(w_ref.at[w], W.at[fs, w], w_send.at[0, w, side], w_recv.at[0, w, side],
                 to_fs(sides[side]))

    def share(kind, k):
        for j in range(1, columns):
            if k == 0:
                src = mine[kind]
            else:
                src = block(kind, tp, level[k])
            send(src, block(kind, tp, level[k]), c_send.at[j, kind, k], c_recv.at[j, kind, k],
                 to_tp(j))

    for kind in range(2):
        share(kind, 0)
        T[kind, pl.ds(pl.multiple_of((tp * 4 + rep) * rows, rows), rows), :] = mine[kind][...]
    W[fs] = w_ref[...]

    for kind in range(2):
        for side in range(2):
            k = 4 - sides[side]
            arrive(block(kind, tp, level[k]), t_send.at[0, kind, side],
                   t_recv.at[0, kind, side], to_rep(sides[side]))
            if kind == side:
                send(block(kind, tp, level[k]), block(kind, tp, level[k]),
                     t_send.at[1, kind, side], t_recv.at[1, kind, side], to_rep(sides[side]))
            share(kind, k)
    for w in range(3):
        for side in range(2):
            f = near[4 - sides[side]]
            arrive(W.at[f, w], w_send.at[0, w, side], w_recv.at[0, w, side], to_fs(sides[side]))
            send(W.at[f, w, :, lanes(side)], W.at[f, w, :, lanes(side)],
                 w_send.at[1, w, side], w_recv.at[1, w, side], to_fs(sides[side]))
    for kind in range(2):
        arrive(block(kind, tp, level[2]), t_send.at[1, kind, kind], t_recv.at[1, kind, kind],
               to_rep(sides[kind]))
        share(kind, 2)
    for kind in range(2):
        for k in range(4):
            for j in range(1, columns):
                arrive(block(kind, core[columns - j], level[k]), c_send.at[j, kind, k],
                       c_recv.at[j, kind, k], to_tp(j))
    for w in range(3):
        for side in range(2):
            arrive(W.at[near[2], w, :, lanes(side)], w_send.at[1, w, side],
                   w_recv.at[1, w, side], to_fs(sides[side]))

    def product(kind, w, at):
        total = None
        for f in range(4):
            piece = lax.dot_general(
                T[kind, at, f * width : (f + 1) * width], W[f, w],
                (((1,), (1,)), ((), ())), preferred_element_type=F32,
            )
            total = piece if total is None else total + piece
        return total.astype(BF).astype(F32)

    def activations(i, carry):
        at = pl.ds(pl.multiple_of(i * tile, tile), tile)
        gate = product(0, 0, at)
        up = product(0, 1, at)
        sigmoid = jax.nn.sigmoid(gate)
        activated = gate * sigmoid
        H[2, at, :] = (activated * up).astype(BF)
        grad = product(1, 2, at)
        H[0, at, :] = (grad * up * sigmoid * (1.0 + gate * (1.0 - sigmoid))).astype(BF)
        H[1, at, :] = (grad * activated).astype(BF)
        return carry

    lax.fori_loop(0, columns, activations, 0)

    def weight_part(w, k):
        at = pl.ds(pl.multiple_of(near[k] * width, width), width)
        return factor * lax.dot_general(
            H[w], T[1 if w == 2 else 0, :, at], (((0,), (0,)), ((), ())),
            preferred_element_type=F32,
        )

    def scatter(w):
        far = weight_part(w, 2).astype(BF)
        for side in range(2):
            S[w, 0, side] = far[:, side * half : (side + 1) * half]
            send(S.at[w, 0, side], RD.at[w, side], d_send.at[w, side], d_recv.at[w, side],
                 to_fs(sides[side]))
        for side in range(2):
            part = weight_part(w, sides[side]).astype(BF)
            for h in range(2):
                S[w, 1 + side, h] = part[:, h * half : (h + 1) * half]
            h = 1 - side
            send(S.at[w, 1 + side, h], RR.at[w, side, h], s_send.at[w, side, h],
                 s_recv.at[w, side, h], to_fs(sides[side]))
        O[w] = weight_part(w, 0)

    def input_part(i, f):
        at = pl.ds(pl.multiple_of(i * tile, tile), tile)
        return jnp.dot(H[0, at, :], W[f, 0], preferred_element_type=F32) + jnp.dot(
            H[1, at, :], W[f, 1], preferred_element_type=F32
        )

    for j in range(1, columns):
        for f in range(4):
            PS[j, :, f * width : (f + 1) * width] = input_part(core[j], f).astype(BF)
        send(PS.at[j], PR.at[j], p_send.at[j], p_recv.at[j], to_tp(j))

    scatter(0)
    for j in range(1, columns):
        arrive(PR.at[j], p_send.at[j], p_recv.at[j], to_tp(j))
    for f in range(4):
        at = slice(f * width, (f + 1) * width)
        total = input_part(tp, f)
        for j in range(1, columns):
            total += PR[j, :, at].astype(F32)
        for r in range(4):
            Q[r, :, at] = total[r * rows : (r + 1) * rows].astype(BF)
    for k in (2, 1, 3):
        send(Q.at[level[k]], QR.at[k], q_send.at[k], q_recv.at[k], to_rep(k))

    scatter(1)
    scatter(2)

    for w in range(3):
        for side in range(2):
            arrive(RD.at[w, side], d_send.at[w, side], d_recv.at[w, side], to_fs(sides[side]))
            S[w, 3 + side, side] = (
                S[w, 1 + side, side].astype(F32) + RD[w, side].astype(F32)
            ).astype(BF)
            send(S.at[w, 3 + side, side], RR.at[w, side, side], s_send.at[w, side, side],
                 s_recv.at[w, side, side], to_fs(sides[side]))

    for w in range(3):
        for side in range(2):
            for h in range(2):
                arrive(RR.at[w, side, h], s_send.at[w, side, h], s_recv.at[w, side, h],
                       to_fs(sides[side]))
        for h in range(2):
            at = slice(h * half, (h + 1) * half)
            G[rep, w, :, at] = (
                O[w, :, at] + RR[w, 0, h].astype(F32) + RR[w, 1, h].astype(F32)
            ).astype(BF)
        for side in range(2):
            send(G.at[rep, w], G.at[rep, w], g_send.at[0, w, side], g_recv.at[0, w, side],
                 to_rep(sides[side]))

    for k in (1, 2, 3):
        arrive(QR.at[k], q_send.at[k], q_recv.at[k], to_rep(k))
    total = Q[rep].astype(F32)
    for k in (1, 2, 3):
        total += QR[k].astype(F32)
    gin_ref[...] = total.astype(BF)

    for w in range(3):
        for side in range(2):
            r = level[4 - sides[side]]
            arrive(G.at[r, w], g_send.at[0, w, side], g_recv.at[0, w, side], to_rep(sides[side]))
            send(G.at[r, w, :, lanes(side)], G.at[r, w, :, lanes(side)],
                 g_send.at[1, w, side], g_recv.at[1, w, side], to_rep(sides[side]))
    for w in range(3):
        for side in range(2):
            arrive(G.at[level[2], w, :, lanes(side)], g_send.at[1, w, side],
                   g_recv.at[1, w, side], to_rep(sides[side]))
        for r in range(4):
            if w == 2:
                gd_ref[r] = G[r, w]
            else:
                gu_ref[w, :, r * part : (r + 1) * part] = G[r, w].astype(F32).T.astype(BF)
    for copy in pending:
        copy.wait_send()


def body(tokens_in, out_grad, gate_weight, up_weight, down_weight):
    replicas = lax.axis_size("rep")
    shards = lax.axis_size("fs")
    columns = lax.axis_size("tp")
    rows, model = tokens_in.shape
    width, hidden_cols = gate_weight.shape
    everyone = rows * replicas * columns
    factor = (everyone * shards) ** (-0.5)
    part = hidden_cols // replicas
    half = width // 2
    offset = lax.axis_index("rep") * part
    pieces = jnp.stack(
        [
            lax.dynamic_slice_in_dim(gate_weight, offset, part, 1).T,
            lax.dynamic_slice_in_dim(up_weight, offset, part, 1).T,
            lax.dynamic_slice_in_dim(down_weight, offset, part, 0),
        ]
    )
    sems = pltpu.SemaphoreType.DMA
    shapes = []
    for dims in ((2, 3, 2), (2, 2, 2), (columns, 2, 4), (3, 2), (3, 2, 2), (2, 3, 2), (columns,), (4,)):
        shapes += [sems(dims), sems(dims)]
    vmem = pl.BlockSpec(memory_space=pltpu.VMEM)
    grad_in, wide, down = pl.pallas_call(
        functools.partial(kernel, columns, factor),
        out_shape=(
            jax.ShapeDtypeStruct((rows, model), BF),
            jax.ShapeDtypeStruct((2, width, hidden_cols), BF),
            jax.ShapeDtypeStruct((4, part, width), BF),
        ),
        in_specs=[vmem] * 3,
        out_specs=(vmem, vmem, vmem),
        scratch_shapes=[
            pltpu.VMEM((2, everyone, model), BF),
            pltpu.VMEM((4, 3, part, width), BF),
            pltpu.VMEM((3, everyone, part), BF),
            pltpu.VMEM((3, 5, 2, part, half), BF),
            pltpu.VMEM((3, part, width), F32),
            pltpu.VMEM((3, 2, part, half), BF),
            pltpu.VMEM((3, 2, 2, part, half), BF),
            pltpu.VMEM((4, 3, part, width), BF),
            pltpu.VMEM((columns, 4 * rows, model), BF),
            pltpu.VMEM((columns, 4 * rows, model), BF),
            pltpu.VMEM((4, rows, model), BF),
            pltpu.VMEM((4, rows, model), BF),
        ]
        + shapes,
        compiler_params=pltpu.CompilerParams(
            collective_id=0, has_side_effects=True, vmem_limit_bytes=60 * 1024 * 1024
        ),
    )(tokens_in, out_grad, pieces)
    return (
        grad_in,
        wide[0].astype(F32),
        wide[1].astype(F32),
        down.reshape(hidden_cols, width).astype(F32),
    )


def contract_last(left, right):
    return lax.dot_general(
        left, right, (((1,), (1,)), ((), ())), preferred_element_type=jnp.float32
    )


def contract_first(left, right):
    return lax.dot_general(
        left, right, (((0,), (0,)), ((), ())), preferred_element_type=jnp.float32
    )


def plain_body(tokens_in, out_grad, gate_weight, up_weight, down_weight):
    replicas = lax.axis_size("rep")
    shards = lax.axis_size("fs")
    columns = lax.axis_size("tp")
    local_rows = tokens_in.shape[0]
    hidden_cols = gate_weight.shape[1]
    factor = (local_rows * replicas * shards * columns) ** (-0.5)
    part = hidden_cols // replicas
    offset = lax.axis_index("rep") * part
    pieces = jnp.stack(
        [
            lax.dynamic_slice_in_dim(gate_weight, offset, part, 1).T,
            lax.dynamic_slice_in_dim(up_weight, offset, part, 1).T,
            lax.dynamic_slice_in_dim(down_weight, offset, part, 0),
        ]
    )
    full = lax.all_gather(pieces, "fs", axis=2, tiled=True)
    gate_full, up_full, down_full = full[0], full[1], full[2]
    both = lax.all_gather(jnp.stack([tokens_in, out_grad]), ("rep", "tp"), axis=1, tiled=True)
    tokens_all, grads_all = both[0], both[1]
    gate = contract_last(tokens_all, gate_full).astype(jnp.bfloat16)
    up_proj = contract_last(tokens_all, up_full).astype(jnp.bfloat16)
    gate_wide = gate.astype(jnp.float32)
    up_wide = up_proj.astype(jnp.float32)
    sigmoid = jax.nn.sigmoid(gate_wide)
    activated = gate_wide * sigmoid
    hidden = (activated * up_wide).astype(jnp.bfloat16)
    grad_hidden = contract_last(grads_all, down_full).astype(jnp.bfloat16)
    grad_wide = grad_hidden.astype(jnp.float32)
    grad_gate = (grad_wide * up_wide * sigmoid * (1.0 + gate_wide * (1.0 - sigmoid))).astype(
        jnp.bfloat16
    )
    grad_up = (grad_wide * activated).astype(jnp.bfloat16)
    weights = factor * jnp.stack(
        [
            contract_first(grad_gate, tokens_all),
            contract_first(grad_up, tokens_all),
            contract_first(hidden, grads_all),
        ]
    )
    owned = lax.psum_scatter(
        weights.astype(jnp.bfloat16), "fs", scatter_dimension=2, tiled=True
    )
    summed = lax.all_gather(owned, "rep", axis=1, tiled=True).astype(jnp.float32)
    partial = jnp.dot(grad_gate, gate_full, preferred_element_type=jnp.float32) + jnp.dot(
        grad_up, up_full, preferred_element_type=jnp.float32
    )
    grad_in = lax.psum_scatter(
        partial.astype(jnp.bfloat16), ("rep", "tp"), scatter_dimension=0, tiled=True
    )
    return (grad_in, summed[0].T, summed[1].T, summed[2])


def solution(mesh):
    placed = (
        P(("rep", "fs", "tp"), None),
        P(("rep", "fs", "tp"), None),
        P("fs", "tp"),
        P("fs", "tp"),
        P("tp", "fs"),
    )
    fits = mesh.shape["rep"] == 4 and mesh.shape["fs"] == 4
    return jax.shard_map(
        body if fits else plain_body,
        mesh=mesh,
        in_specs=placed,
        out_specs=(P(("rep", "fs", "tp"), None), P("fs", "tp"), P("fs", "tp"), P("tp", "fs")),
        check_vma=False,
    )
```
